32 devices in a mesh: fs: 8 (over z, y), tp: 4 (over x, core).
Axes of the slice: x: 2, y: 2, z: 4, core: 2. Of those that a mesh axis runs over, the one named last changes fastest.
Arguments:
- stream: bfloat16 [4096, 1024], P(('fs', 'tp')), may hold values from -3 to 3
- mixer_out: bfloat16 [4096, 1024], P(('fs', 'tp')), may hold values from -6 to 6
- ffn_gains: float32 [4, 1024], replicated, may hold values from 0.5 to 1.5
- mixer_gain: float32 [1024], replicated, may hold values from 0.25 to 0.6
- gate_first: bfloat16 [1024, 2816], P('fs', 'tp'), may hold values from -0.1875 to 0.1875
- up_first: bfloat16 [1024, 2816], P('fs', 'tp'), may hold values from -0.1875 to 0.1875
- down_first: bfloat16 [2816, 1024], P('tp', 'fs'), may hold values from -0.109375 to 0.109375
- gate_second: bfloat16 [1024, 2816], P('fs', 'tp'), may hold values from -0.1875 to 0.1875
- up_second: bfloat16 [1024, 2816], P('fs', 'tp'), may hold values from -0.1875 to 0.1875
- down_second: bfloat16 [2816, 1024], P('tp', 'fs'), may hold values from -0.109375 to 0.109375
Outputs:
- layer_out: bfloat16 [4096, 1024], P(('fs', 'tp'))
The draws below stay inside these ranges and needn't reach their ends.
All inputs are finite; a program needn't handle non-finite values.
Results may differ from the reference program's by a relative error of at most 0.02.
Values may be sent and summed in bfloat16 or wider, within the bound.
A program may use at most 64 MiB of HBM per device.

```python
import jax
import jax.numpy as jnp
from jax import lax

D = 1024
FF = 2816
TOK_DEV = 128
TOKENS = 4096
N_FS = 8
N_TP = 4


def levels(stream_key, dims, split, smallest, largest):
    def one(axis_at, parts):
        draws = jax.random.uniform(jax.random.fold_in(jax.random.fold_in(stream_key, 6), axis_at), (parts,), jnp.float32, smallest / len(split), largest / len(split))
        return jnp.repeat(jnp.exp(draws), dims[axis_at] // parts).reshape((-1,) + (1,) * (len(dims) - axis_at - 1))

    level = one(*split[0])
    for cut in split[1:]:
        level = level * one(*cut)
    return level


def bell_draw(own_key, shape, width, reach, pieces=(), kind=jnp.bfloat16):
    loudness = levels(own_key, shape, pieces, -0.22, 0.18) if pieces else 1.0
    drawn = jax.random.normal(own_key, shape, jnp.float32) * width * loudness
    return jnp.minimum(jnp.maximum(drawn, -reach), reach).astype(kind)


def setup_inputs(seed: int = 0) -> dict:
    key_of = jax.random.split(jax.random.key(seed), 11)
    return {
        "stream": bell_draw(key_of[0], (TOKENS, D), 0.5, 3.0, ((0, 32),)),
        "mixer_out": bell_draw(key_of[1], (TOKENS, D), 1.0, 6.0, ((0, 32),)),
        "ffn_gains": jnp.clip(1.0 + 0.1 * jax.random.normal(key_of[2], (4, D), jnp.float32), 0.5, 1.5),
        "mixer_gain": jnp.clip(jax.random.uniform(key_of[3], (D,), jnp.float32, 0.25, 0.6), 0.25, 0.6),
        "gate_first": bell_draw(key_of[4], (D, FF), D ** -0.5, 0.1875, ((0, 8), (1, 4))),
        "up_first": bell_draw(key_of[5], (D, FF), D ** -0.5, 0.1875, ((0, 8), (1, 4))),
        "down_first": bell_draw(key_of[6], (FF, D), FF ** -0.5, 0.109375, ((0, 4), (1, 8))),
        "gate_second": bell_draw(key_of[7], (D, FF), D ** -0.5, 0.1875, ((0, 8), (1, 4))),
        "up_second": bell_draw(key_of[8], (D, FF), D ** -0.5, 0.1875, ((0, 8), (1, 4))),
        "down_second": bell_draw(key_of[9], (FF, D), FF ** -0.5, 0.109375, ((0, 4), (1, 8))),
    }


epsilon = 1e-06
half_weight = 0.5

def rms_rows(values, gain_row):
    widened = values.astype(jnp.float32)
    inverse_rms = lax.rsqrt(lax.optimization_barrier(jnp.mean(widened * widened, axis=-1, keepdims=True)) + epsilon)
    return (widened * inverse_rms * gain_row.astype(jnp.float32)).astype(jnp.bfloat16)

def add_branch(rows, normed_branch, factor):
    return (rows.astype(jnp.float32) + factor * normed_branch.astype(jnp.float32)).astype(jnp.bfloat16)

def half_step(rows, gain_pre, gain_post, gate_w, up_w, down_w):
    normed = rms_rows(rows, gain_pre)
    blocks = normed.reshape(N_FS, TOK_DEV * N_TP, D)

    def feed_block(row_block):
        gate_sum = jnp.dot(row_block, gate_w, preferred_element_type=jnp.float32)
        up_sum = jnp.dot(row_block, up_w, preferred_element_type=jnp.float32)
        hidden = (jax.nn.silu(gate_sum) * up_sum).astype(jnp.bfloat16)
        return jnp.dot(hidden, down_w, preferred_element_type=jnp.float32).astype(jnp.bfloat16)
    branch = lax.map(feed_block, blocks).reshape(TOKENS, D)
    return add_branch(rows, rms_rows(branch, gain_post), half_weight)

def reference(stream, mixer_out, ffn_gains, mixer_gain, gate_first, up_first, down_first, gate_second, up_second, down_second):
    after_first = half_step(stream, ffn_gains[0], ffn_gains[1], gate_first, up_first, down_first)
    mixed_in = add_branch(after_first, rms_rows(mixer_out, mixer_gain), 1.0)
    return half_step(mixed_in, ffn_gains[2], ffn_gains[3], gate_second, up_second, down_second)
```

```python
import functools
import math

import jax
import jax.numpy as jnp
from jax import lax
from jax.experimental import pallas as pl
from jax.experimental.pallas import tpu as pltpu
from jax.sharding import PartitionSpec as P

epsilon = 1e-06
half_weight = 0.5
CORES = 2
PAIR = 2
MESH = pl.DeviceIdType.MESH


def rms_rows(values, gain_row):
    widened = values.astype(jnp.float32)
    inverse_rms = lax.rsqrt(jnp.mean(widened * widened, axis=-1, keepdims=True) + epsilon)
    return (widened * inverse_rms * gain_row).astype(jnp.bfloat16)


def add_branch(rows, normed_branch, factor):
    return (rows.astype(jnp.float32) + factor * normed_branch.astype(jnp.float32)).astype(
        jnp.bfloat16
    )


def layer_kernel(
    dims,
    stream_ref, mixer_ref, gains_ref, mixer_gain_ref, gu1_ref, d1_ref, gu2_ref, d2_ref,
    out_ref,
    gu_all, dn_all, tok, hid, part, psend, rcore, sums, rx, up_sum, rp, mixed,
    zs, zr, ys, yr, gps, gpr, gxs, gxr, gcs, gcr, rcs, rcr, rxs, rxr, rps, rpr, loc,
):
    Z, Y, X, PP, H, HP = dims
    rows = stream_ref.shape[0]
    f, t = lax.axis_index("fs"), lax.axis_index("tp")
    z, y = f // Y, f % Y
    x, c = t // CORES, t % CORES
    p, q = z % PP, z // PP
    gu_in, d_in = (gu1_ref, gu2_ref), (d1_ref, d2_ref)
    alls = (gu_all, dn_all)
    ins = (gu_in, d_in)

    def fs_of(z_to, y_to):
        return z_to * Y + y_to

    def p_peer(kp):
        return (fs_of(q * PP + (p + kp) % PP, y), t)

    def x_peer(kx):
        return (f, ((x + kx) % X) * CORES + c)

    sibling = (f, x * CORES + 1 - c)
    sent = []

    def send(src, dst, s_sem, r_sem, device):
        d = pltpu.make_async_remote_copy(
            src_ref=src, dst_ref=dst, send_sem=s_sem, recv_sem=r_sem,
            device_id=device, device_id_type=MESH,
        )
        d.start()
        sent.append(d)

    def arrived(dst, s_sem, r_sem):
        pltpu.make_async_remote_copy(
            src_ref=dst, dst_ref=dst, send_sem=s_sem, recv_sem=r_sem,
            device_id=sibling, device_id_type=MESH,
        ).wait_recv()

    barrier = pltpu.get_barrier_semaphore()
    peers = [(fs_of((z + k) % Z, y), t) for k in range(1, Z)]
    peers += [(fs_of(z, (y + j) % Y), t) for j in range(1, Y)]
    peers += [x_peer(k) for k in range(1, X)] + [sibling]
    for peer in peers:
        pl.semaphore_signal(barrier, inc=1, device_id=peer, device_id_type=MESH)
    pl.semaphore_wait(barrier, len(peers))

    def z_send(layer, kind):
        for k in range(1, Z):
            dz = (z + k) % Z
            send(ins[kind][layer].at[dz % PP], alls[kind].at[layer, f],
                 zs.at[layer, kind, k], zr.at[layer, kind, k], (fs_of(dz, y), t))

    def y_send(layer, kind, k):
        slot = fs_of((z - k + Z) % Z, y)
        src = ins[kind][layer].at[p] if k == 0 else alls[kind].at[layer, slot]
        if k:
            arrived(alls[kind].at[layer, slot], zs.at[layer, kind, k], zr.at[layer, kind, k])
        for j in range(1, Y):
            send(src, alls[kind].at[layer, slot],
                 ys.at[layer, kind, k, j], yr.at[layer, kind, k, j],
                 (fs_of(z, (y + j) % Y), t))

    def y_wait(layer, kind):
        for k in range(Z):
            for j in range(1, Y):
                slot = fs_of((z - k + Z) % Z, (y - j + Y) % Y)
                arrived(alls[kind].at[layer, slot],
                        ys.at[layer, kind, k, j], yr.at[layer, kind, k, j])

    def forward(layer, kind):
        for k in range(1, Z):
            y_send(layer, kind, k)

    locals_ = []
    for layer in range(2):
        for kind in range(2):
            d = pltpu.make_async_copy(ins[kind][layer].at[p], alls[kind].at[layer, f],
                                      loc.at[layer, kind])
            d.start()
            locals_.append(d)

    def tok_at(phase, kp, kx, core):
        g = (((p - kp + PP) % PP) * X + (x - kx + X) % X) * CORES + core
        return tok.at[phase, pl.ds(pl.multiple_of(g * rows, rows), rows)]

    def gather_x(phase, kp):
        for kx in range(1, X):
            send(tok_at(phase, kp, 0, c), tok_at(phase, kp, 0, c),
                 gxs.at[phase, kp, kx], gxr.at[phase, kp, kx], x_peer(kx))

    def gather_c(phase, kp, kx):
        send(tok_at(phase, kp, kx, c), tok_at(phase, kp, kx, c),
             gcs.at[phase, kp, kx], gcr.at[phase, kp, kx], sibling)

    def gather_start(phase):
        for kp in range(1, PP):
            send(tok_at(phase, 0, 0, c), tok_at(phase, 0, 0, c),
                 gps.at[phase, kp], gpr.at[phase, kp], p_peer(kp))
        gather_x(phase, 0)
        gather_c(phase, 0, 0)

    def gather_relay(phase):
        for kp in range(1, PP):
            arrived(tok_at(phase, kp, 0, c), gps.at[phase, kp], gpr.at[phase, kp])
            gather_x(phase, kp)
            gather_c(phase, kp, 0)

    def gather_cross(phase):
        for kp in range(PP):
            for kx in range(1, X):
                arrived(tok_at(phase, kp, kx, c),
                        gxs.at[phase, kp, kx], gxr.at[phase, kp, kx])
                gather_c(phase, kp, kx)

    def gather_end(phase):
        for kp in range(PP):
            for kx in range(X):
                arrived(tok_at(phase, kp, kx, 1 - c),
                        gcs.at[phase, kp, kx], gcr.at[phase, kp, kx])

    both = CORES * rows

    def gate_up(layer):
        def step(i, carry):
            at = pl.ds(pl.multiple_of(i * both, both), both)
            weights = gu_all[layer].reshape(-1, 2 * HP)
            gu = jnp.dot(tok[layer, at, :], weights, preferred_element_type=jnp.float32)
            gate, value = gu[:, :HP], gu[:, HP:]
            hid[at, :] = (gate / (1.0 + jnp.exp(-gate)) * value).astype(jnp.bfloat16)
            return carry
        lax.fori_loop(0, PP * X, step, 0)

    order = [(kp, kx) for kp in reversed(range(PP)) for kx in reversed(range(X))]

    def project(layer):
        for kp, kx in order:
            o = kp * X + kx
            i = ((p + kp) % PP) * X + (x + kx) % X
            block = hid[pl.ds(pl.multiple_of(i * both, both), both), :][:, :H]
            down = jnp.concatenate([dn_all[layer, s] for s in range(Z * Y)], axis=1)
            res = jnp.dot(block, down, preferred_element_type=jnp.float32)
            low, high = res[:rows], res[rows:]
            part[o] = jnp.where(c == 0, low, high)
            psend[layer, o] = jnp.where(c == 0, high, low).astype(jnp.bfloat16)
            send(psend.at[layer, o], rcore.at[layer, o], rcs.at[layer, o], rcr.at[layer, o],
                 sibling)

    def reduce_core(layer):
        for kp, kx in order:
            o = kp * X + kx
            arrived(rcore.at[layer, o], rcs.at[layer, o], rcr.at[layer, o])
            total = part[o] + rcore[layer, o].astype(jnp.float32)
            if kx == 0:
                part[o] = total
            else:
                sums[layer, o] = total.astype(jnp.bfloat16)
                send(sums.at[layer, o], rx.at[layer, o], rxs.at[layer, o], rxr.at[layer, o],
                     x_peer(kx))

    def reduce_x(layer):
        for kp in reversed(range(PP)):
            total = part[kp * X]
            for kx in range(1, X):
                o = kp * X + kx
                arrived(rx.at[layer, o], rxs.at[layer, o], rxr.at[layer, o])
                total = total + rx[layer, o].astype(jnp.float32)
            if kp == 0:
                part[0] = total
            else:
                up_sum[layer, kp] = total.astype(jnp.bfloat16)
                send(up_sum.at[layer, kp], rp.at[layer, kp], rps.at[layer, kp],
                     rpr.at[layer, kp], p_peer(kp))

    def reduce_p(layer):
        total = part[0]
        for kp in range(1, PP):
            arrived(rp.at[layer, kp], rps.at[layer, kp], rpr.at[layer, kp])
            total = total + rp[layer, kp].astype(jnp.float32)
        return total.astype(jnp.bfloat16)

    own_rows = pl.ds(pl.multiple_of(((p * X + x) * CORES + c) * rows, rows), rows)

    z_send(0, 0)
    y_send(0, 0, 0)
    tok[0, own_rows, :] = rms_rows(stream_ref[...], gains_ref[0:1, :])
    gather_start(0)
    z_send(0, 1)
    y_send(0, 1, 0)
    gather_relay(0)
    forward(0, 0)
    gather_cross(0)
    z_send(1, 0)
    y_send(1, 0, 0)
    for d in locals_:
        d.wait()
    gather_end(0)
    forward(0, 1)
    y_wait(0, 0)
    gate_up(0)
    y_wait(0, 1)
    project(0)
    reduce_core(0)
    reduce_x(0)
    z_send(1, 1)
    y_send(1, 1, 0)
    branch = reduce_p(0)
    after_first = add_branch(
        stream_ref[...], rms_rows(branch, gains_ref[1:2, :]), half_weight
    )
    joined = add_branch(after_first, rms_rows(mixer_ref[...], mixer_gain_ref[...]), 1.0)
    mixed[...] = joined
    tok[1, own_rows, :] = rms_rows(joined, gains_ref[2:3, :])
    gather_start(1)
    gather_relay(1)
    forward(1, 0)
    gather_cross(1)
    gather_end(1)
    forward(1, 1)
    y_wait(1, 0)
    gate_up(1)
    y_wait(1, 1)
    project(1)
    reduce_core(1)
    reduce_x(1)
    branch_two = reduce_p(1)
    out_ref[...] = add_branch(
        mixed[...], rms_rows(branch_two, gains_ref[3:4, :]), half_weight
    )
    for d in sent:
        d.wait_send()


def on_device(sizes, stream, mixer_out, ffn_gains, mixer_gain,
              gate_first, up_first, down_first, gate_second, up_second, down_second):
    n_fs, n_tp = sizes
    X = n_tp // CORES
    Y = math.gcd(n_fs, X)
    Z = n_fs // Y
    PP = math.gcd(Z, PAIR)
    depth, local_h = gate_first.shape
    H = local_h // PP
    HP = -(-H // 128) * 128
    rows, width = stream.shape

    def halves(gate, up):
        def cut(w):
            w = w.reshape(depth, PP, H).transpose(1, 0, 2)
            return jnp.pad(w, ((0, 0), (0, 0), (0, HP - H)))
        return jnp.concatenate([cut(gate), cut(up)], axis=2)

    def rows_cut(down):
        return down.reshape(PP, H, down.shape[1])

    group = PP * X
    bf, f32 = jnp.bfloat16, jnp.float32
    dma = pltpu.SemaphoreType.DMA
    vm = pltpu.VMEM
    F = n_fs
    scratch = [
        vm((2, F, depth, 2 * HP), bf), vm((2, F, H, depth), bf),
        vm((2, group * CORES * rows, width), bf), vm((group * CORES * rows, HP), bf),
        vm((group, rows, width), f32), vm((2, group, rows, width), bf),
        vm((2, group, rows, width), bf), vm((2, group, rows, width), bf),
        vm((2, group, rows, width), bf), vm((2, PP, rows, width), bf),
        vm((2, PP, rows, width), bf), vm((rows, width), bf),
        dma((2, 2, Z)), dma((2, 2, Z)), dma((2, 2, Z, Y)), dma((2, 2, Z, Y)),
        dma((2, PP)), dma((2, PP)), dma((2, PP, X)), dma((2, PP, X)),
        dma((2, PP, X)), dma((2, PP, X)), dma((2, group)), dma((2, group)),
        dma((2, group)), dma((2, group)), dma((2, PP)), dma((2, PP)), dma((2, 2)),
    ]
    return pl.pallas_call(
        functools.partial(layer_kernel, (Z, Y, X, PP, H, HP)),
        out_shape=jax.ShapeDtypeStruct((rows, width), bf),
        in_specs=[pl.BlockSpec(memory_space=vm)] * 8,
        out_specs=pl.BlockSpec(memory_space=vm),
        scratch_shapes=scratch,
        compiler_params=pltpu.CompilerParams(collective_id=0, has_side_effects=True),
        name="macaron",
    )(stream, mixer_out, ffn_gains, mixer_gain.reshape(1, -1),
      halves(gate_first, up_first), rows_cut(down_first),
      halves(gate_second, up_second), rows_cut(down_second))


def solution(mesh):
    in_specs = (
        P(("fs", "tp"), None), P(("fs", "tp"), None), P(), P(),
        P("fs", "tp"), P("fs", "tp"), P("tp", "fs"),
        P("fs", "tp"), P("fs", "tp"), P("tp", "fs"),
    )
    sizes = (mesh.shape["fs"], mesh.shape["tp"])
    return jax.shard_map(
        functools.partial(on_device, sizes), mesh=mesh, in_specs=in_specs,
        out_specs=P(("fs", "tp"), None), check_vma=False,
    )
```

```python
import functools
import math

import jax
import jax.numpy as jnp
from jax import lax
from jax.experimental import pallas as pl
from jax.experimental.pallas import tpu as pltpu
from jax.sharding import PartitionSpec as P

epsilon = 1e-06
half_weight = 0.5
CORES = 2
PAIR = 2
MESH = pl.DeviceIdType.MESH


def rms_rows(values, gain_row):
    widened = values.astype(jnp.float32)
    inverse_rms = lax.rsqrt(jnp.mean(widened * widened, axis=-1, keepdims=True) + epsilon)
    return (widened * inverse_rms * gain_row).astype(jnp.bfloat16)


def add_branch(rows, normed_branch, factor):
    return (rows.astype(jnp.float32) + factor * normed_branch.astype(jnp.float32)).astype(
        jnp.bfloat16
    )


def layer_kernel(
    dims,
    stream_hbm, mixer_hbm, gains_ref, mixer_gain_ref,
    g1_hbm, u1_hbm, d1_ref, g2_hbm, u2_hbm, d2_ref,
    out_ref,
    stream_ref, mixer_ref, raw, gu_in, gu_all, dn_all, tok, hid, part, psend, rcore, sums, rx, up_sum, rp, mixed,
    zs, zr, ys, yr, gps, gpr, gxs, gxr, gcs, gcr, rcs, rcr, rxs, rxr, rps, rpr, loc, lin,
):
    Z, Y, X, PP, H, HP = dims
    rows = stream_ref.shape[0]
    depth = raw.shape[2]
    f, t = lax.axis_index("fs"), lax.axis_index("tp")
    z, y = f // Y, f % Y
    x, c = t // CORES, t % CORES
    p, q = z % PP, z // PP
    d_in = (d1_ref, d2_ref)
    alls = (gu_all, dn_all)

    def half_of(kind, layer, which):
        if kind == 0:
            return gu_in.at[layer, which]
        return d_in[layer].at[pl.ds(pl.multiple_of(which * H, 16), H)]

    loads = []
    for n, (src, dst) in enumerate((
        (stream_hbm, stream_ref), (g1_hbm, raw.at[0, 0]), (u1_hbm, raw.at[0, 1]),
        (g2_hbm, raw.at[1, 0]), (u2_hbm, raw.at[1, 1]), (mixer_hbm, mixer_ref),
    )):
        d = pltpu.make_async_copy(src, dst, lin.at[n])
        d.start()
        loads.append(d)

    def pack(layer):
        fill = jnp.zeros((depth, HP - H), jnp.bfloat16)
        for side in range(2):
            w = raw[layer, side]
            for which in range(PP):
                cut = w[:, which * H:(which + 1) * H]
                if HP > H:
                    cut = jnp.concatenate([cut, fill], axis=1)
                gu_in[layer, which, :, side * HP:(side + 1) * HP] = cut

    def fs_of(z_to, y_to):
        return z_to * Y + y_to

    def p_peer(kp):
        return (fs_of(q * PP + (p + kp) % PP, y), t)

    def x_peer(kx):
        return (f, ((x + kx) % X) * CORES + c)

    sibling = (f, x * CORES + 1 - c)
    sent = []

    def send(src, dst, s_sem, r_sem, device):
        d = pltpu.make_async_remote_copy(
            src_ref=src, dst_ref=dst, send_sem=s_sem, recv_sem=r_sem,
            device_id=device, device_id_type=MESH,
        )
        d.start()
        sent.append(d)

    def arrived(dst, s_sem, r_sem):
        pltpu.make_async_remote_copy(
            src_ref=dst, dst_ref=dst, send_sem=s_sem, recv_sem=r_sem,
            device_id=sibling, device_id_type=MESH,
        ).wait_recv()

    barrier = pltpu.get_barrier_semaphore()
    peers = [(fs_of((z + k) % Z, y), t) for k in range(1, Z)]
    peers += [(fs_of(z, (y + j) % Y), t) for j in range(1, Y)]
    peers += [x_peer(k) for k in range(1, X)] + [sibling]
    for peer in peers:
        pl.semaphore_signal(barrier, inc=1, device_id=peer, device_id_type=MESH)
    pl.semaphore_wait(barrier, len(peers))

    def z_send(layer, kind):
        for k in range(1, Z):
            dz = (z + k) % Z
            send(half_of(kind, layer, dz % PP), alls[kind].at[layer, f],
                 zs.at[layer, kind, k], zr.at[layer, kind, k], (fs_of(dz, y), t))

    def y_send(layer, kind, k):
        slot = fs_of((z - k + Z) % Z, y)
        src = half_of(kind, layer, p) if k == 0 else alls[kind].at[layer, slot]
        if k:
            arrived(alls[kind].at[layer, slot], zs.at[layer, kind, k], zr.at[layer, kind, k])
        for j in range(1, Y):
            send(src, alls[kind].at[layer, slot],
                 ys.at[layer, kind, k, j], yr.at[layer, kind, k, j],
                 (fs_of(z, (y + j) % Y), t))

    def y_wait(layer, kind):
        for k in range(Z):
            for j in range(1, Y):
                slot = fs_of((z - k + Z) % Z, (y - j + Y) % Y)
                arrived(alls[kind].at[layer, slot],
                        ys.at[layer, kind, k, j], yr.at[layer, kind, k, j])

    def forward(layer, kind):
        for k in range(1, Z):
            y_send(layer, kind, k)

    locals_ = []

    def keep_own(layer):
        for kind in range(2):
            d = pltpu.make_async_copy(half_of(kind, layer, p), alls[kind].at[layer, f],
                                      loc.at[layer, kind])
            d.start()
            locals_.append(d)

    def tok_at(phase, kp, kx, core):
        g = (((p - kp + PP) % PP) * X + (x - kx + X) % X) * CORES + core
        return tok.at[phase, pl.ds(pl.multiple_of(g * rows, rows), rows)]

    def gather_x(phase, kp):
        for kx in range(1, X):
            send(tok_at(phase, kp, 0, c), tok_at(phase, kp, 0, c),
                 gxs.at[phase, kp, kx], gxr.at[phase, kp, kx], x_peer(kx))

    def gather_c(phase, kp, kx):
        send(tok_at(phase, kp, kx, c), tok_at(phase, kp, kx, c),
             gcs.at[phase, kp, kx], gcr.at[phase, kp, kx], sibling)

    def gather_start(phase):
        for kp in range(1, PP):
            send(tok_at(phase, 0, 0, c), tok_at(phase, 0, 0, c),
                 gps.at[phase, kp], gpr.at[phase, kp], p_peer(kp))
        gather_x(phase, 0)
        gather_c(phase, 0, 0)

    def gather_relay(phase):
        for kp in range(1, PP):
            arrived(tok_at(phase, kp, 0, c), gps.at[phase, kp], gpr.at[phase, kp])
            gather_x(phase, kp)
            gather_c(phase, kp, 0)

    def gather_cross(phase):
        for kp in range(PP):
            for kx in range(1, X):
                arrived(tok_at(phase, kp, kx, c),
                        gxs.at[phase, kp, kx], gxr.at[phase, kp, kx])
                gather_c(phase, kp, kx)

    def gather_end(phase):
        for kp in range(PP):
            for kx in range(X):
                arrived(tok_at(phase, kp, kx, 1 - c),
                        gcs.at[phase, kp, kx], gcr.at[phase, kp, kx])

    both = CORES * rows

    def gate_up(layer):
        def step(i, carry):
            at = pl.ds(pl.multiple_of(i * both, both), both)
            weights = gu_all[layer].reshape(-1, 2 * HP)
            gu = jnp.dot(tok[layer, at, :], weights, preferred_element_type=jnp.float32)
            gate, value = gu[:, :HP], gu[:, HP:]
            hid[at, :] = (gate / (1.0 + jnp.exp(-gate)) * value).astype(jnp.bfloat16)
            return carry
        lax.fori_loop(0, PP * X, step, 0)

    order = [(kp, kx) for kp in reversed(range(PP)) for kx in reversed(range(X))]

    def project(layer):
        for kp, kx in order:
            o = kp * X + kx
            i = ((p + kp) % PP) * X + (x + kx) % X
            block = hid[pl.ds(pl.multiple_of(i * both, both), both), :][:, :H]
            down = jnp.concatenate([dn_all[layer, s] for s in range(Z * Y)], axis=1)
            res = jnp.dot(block, down, preferred_element_type=jnp.float32)
            low, high = res[:rows], res[rows:]
            part[o] = jnp.where(c == 0, low, high)
            psend[layer, o] = jnp.where(c == 0, high, low).astype(jnp.bfloat16)
            send(psend.at[layer, o], rcore.at[layer, o], rcs.at[layer, o], rcr.at[layer, o],
                 sibling)

    def reduce_core(layer):
        for kp, kx in order:
            o = kp * X + kx
            arrived(rcore.at[layer, o], rcs.at[layer, o], rcr.at[layer, o])
            total = part[o] + rcore[layer, o].astype(jnp.float32)
            if kx == 0:
                part[o] = total
            else:
                sums[layer, o] = total.astype(jnp.bfloat16)
                send(sums.at[layer, o], rx.at[layer, o], rxs.at[layer, o], rxr.at[layer, o],
                     x_peer(kx))

    def reduce_x(layer):
        for kp in reversed(range(PP)):
            total = part[kp * X]
            for kx in range(1, X):
                o = kp * X + kx
                arrived(rx.at[layer, o], rxs.at[layer, o], rxr.at[layer, o])
                total = total + rx[layer, o].astype(jnp.float32)
            if kp == 0:
                part[0] = total
            else:
                up_sum[layer, kp] = total.astype(jnp.bfloat16)
                send(up_sum.at[layer, kp], rp.at[layer, kp], rps.at[layer, kp],
                     rpr.at[layer, kp], p_peer(kp))

    def reduce_p(layer):
        total = part[0]
        for kp in range(1, PP):
            arrived(rp.at[layer, kp], rps.at[layer, kp], rpr.at[layer, kp])
            total = total + rp[layer, kp].astype(jnp.float32)
        return total.astype(jnp.bfloat16)

    own_rows = pl.ds(pl.multiple_of(((p * X + x) * CORES + c) * rows, rows), rows)

    loads[0].wait()
    tok[0, own_rows, :] = rms_rows(stream_ref[...], gains_ref[0:1, :])
    gather_start(0)
    loads[1].wait()
    loads[2].wait()
    pack(0)
    z_send(0, 0)
    y_send(0, 0, 0)
    z_send(0, 1)
    y_send(0, 1, 0)
    keep_own(0)
    loads[3].wait()
    loads[4].wait()
    pack(1)
    z_send(1, 0)
    z_send(1, 1)
    keep_own(1)
    gather_relay(0)
    gather_cross(0)
    forward(0, 0)
    gather_end(0)
    forward(0, 1)
    y_send(1, 0, 0)
    y_send(1, 1, 0)
    loads[5].wait()
    for d in locals_:
        d.wait()
    y_wait(0, 0)
    gate_up(0)
    y_wait(0, 1)
    project(0)
    reduce_core(0)
    forward(1, 0)
    reduce_x(0)
    forward(1, 1)
    branch = reduce_p(0)
    after_first = add_branch(
        stream_ref[...], rms_rows(branch, gains_ref[1:2, :]), half_weight
    )
    joined = add_branch(after_first, rms_rows(mixer_ref[...], mixer_gain_ref[...]), 1.0)
    mixed[...] = joined
    tok[1, own_rows, :] = rms_rows(joined, gains_ref[2:3, :])
    gather_start(1)
    gather_relay(1)
    gather_cross(1)
    gather_end(1)
    y_wait(1, 0)
    gate_up(1)
    y_wait(1, 1)
    project(1)
    reduce_core(1)
    reduce_x(1)
    branch_two = reduce_p(1)
    out_ref[...] = add_branch(
        mixed[...], rms_rows(branch_two, gains_ref[3:4, :]), half_weight
    )
    for d in sent:
        d.wait_send()


def on_device(sizes, stream, mixer_out, ffn_gains, mixer_gain,
              gate_first, up_first, down_first, gate_second, up_second, down_second):
    n_fs, n_tp = sizes
    X = n_tp // CORES
    Y = math.gcd(n_fs, X)
    Z = n_fs // Y
    PP = math.gcd(Z, PAIR)
    depth, local_h = gate_first.shape
    H = local_h // PP
    HP = -(-H // 128) * 128
    rows, width = stream.shape

    group = PP * X
    bf, f32 = jnp.bfloat16, jnp.float32
    dma = pltpu.SemaphoreType.DMA
    vm = pltpu.VMEM
    F = n_fs
    any_ = pl.ANY
    scratch = [
        vm((rows, width), bf), vm((rows, width), bf), vm((2, 2, depth, local_h), bf),
        vm((2, PP, depth, 2 * HP), bf),
        vm((2, F, depth, 2 * HP), bf), vm((2, F, H, depth), bf),
        vm((2, group * CORES * rows, width), bf), vm((group * CORES * rows, HP), bf),
        vm((group, rows, width), f32), vm((2, group, rows, width), bf),
        vm((2, group, rows, width), bf), vm((2, group, rows, width), bf),
        vm((2, group, rows, width), bf), vm((2, PP, rows, width), bf),
        vm((2, PP, rows, width), bf), vm((rows, width), bf),
        dma((2, 2, Z)), dma((2, 2, Z)), dma((2, 2, Z, Y)), dma((2, 2, Z, Y)),
        dma((2, PP)), dma((2, PP)), dma((2, PP, X)), dma((2, PP, X)),
        dma((2, PP, X)), dma((2, PP, X)), dma((2, group)), dma((2, group)),
        dma((2, group)), dma((2, group)), dma((2, PP)), dma((2, PP)), dma((2, 2)), dma((6,)),
    ]
    return pl.pallas_call(
        functools.partial(layer_kernel, (Z, Y, X, PP, H, HP)),
        out_shape=jax.ShapeDtypeStruct((rows, width), bf),
        in_specs=[pl.BlockSpec(memory_space=m) for m in (any_, any_, vm, vm) + (any_,) * 6],
        out_specs=pl.BlockSpec(memory_space=vm),
        scratch_shapes=scratch,
        compiler_params=pltpu.CompilerParams(collective_id=0, has_side_effects=True),
        name="macaron",
    )(stream, mixer_out, ffn_gains, mixer_gain.reshape(1, -1),
      gate_first, up_first, down_first, gate_second, up_second, down_second)


def solution(mesh):
    in_specs = (
        P(("fs", "tp"), None), P(("fs", "tp"), None), P(), P(),
        P("fs", "tp"), P("fs", "tp"), P("tp", "fs"),
        P("fs", "tp"), P("fs", "tp"), P("tp", "fs"),
    )
    sizes = (mesh.shape["fs"], mesh.shape["tp"])
    return jax.shard_map(
        functools.partial(on_device, sizes), mesh=mesh, in_specs=in_specs,
        out_specs=P(("fs", "tp"), None), check_vma=False,
    )
```

```python
import functools
import math

import jax
import jax.numpy as jnp
from jax import lax
from jax.experimental import pallas as pl
from jax.experimental.pallas import tpu as pltpu
from jax.sharding import PartitionSpec as P

epsilon = 1e-06
half_weight = 0.5
CORES = 2
PAIR = 2
MESH = pl.DeviceIdType.MESH


def rms_rows(values, gain_row):
    widened = values.astype(jnp.float32)
    inverse_rms = lax.rsqrt(jnp.mean(widened * widened, axis=-1, keepdims=True) + epsilon)
    return (widened * inverse_rms * gain_row).astype(jnp.bfloat16)


def add_branch(rows, normed_branch, factor):
    return (rows.astype(jnp.float32) + factor * normed_branch.astype(jnp.float32)).astype(
        jnp.bfloat16
    )


def layer_kernel(
    dims,
    stream_hbm, mixer_hbm, gains_ref, mixer_gain_ref,
    g1_hbm, u1_hbm, d1_ref, g2_hbm, u2_hbm, d2_ref,
    out_ref,
    stream_ref, mixer_ref, raw, gu_in, gu_all, dn_all, tok, hid, part, psend, rcore, sums, rx, up_sum, rp, mixed,
    zs, zr, ys, yr, gps, gpr, gxs, gxr, gcs, gcr, rcs, rcr, rxs, rxr, rps, rpr, loc, lin,
):
    Z, Y, X, PP, H, HP = dims
    rows = stream_ref.shape[0]
    depth = raw.shape[2]
    f, t = lax.axis_index("fs"), lax.axis_index("tp")
    z, y = f // Y, f % Y
    x, c = t // CORES, t % CORES
    p, q = z % PP, z // PP
    d_in = (d1_ref, d2_ref)
    alls = (gu_all, dn_all)

    def half_of(kind, layer, which):
        if kind == 0:
            return gu_in.at[layer, which]
        return d_in[layer].at[pl.ds(pl.multiple_of(which * H, 16), H)]

    loads = []
    for n, (src, dst) in enumerate((
        (stream_hbm, stream_ref), (g1_hbm, raw.at[0, 0]), (u1_hbm, raw.at[0, 1]),
        (g2_hbm, raw.at[1, 0]), (u2_hbm, raw.at[1, 1]), (mixer_hbm, mixer_ref),
    )):
        d = pltpu.make_async_copy(src, dst, lin.at[n])
        d.start()
        loads.append(d)

    def pack(layer):
        fill = jnp.zeros((depth, HP - H), jnp.bfloat16)
        for side in range(2):
            w = raw[layer, side]
            for which in range(PP):
                cut = w[:, which * H:(which + 1) * H]
                if HP > H:
                    cut = jnp.concatenate([cut, fill], axis=1)
                gu_in[layer, which, :, side * HP:(side + 1) * HP] = cut

    def fs_of(z_to, y_to):
        return z_to * Y + y_to

    def p_peer(kp):
        return (fs_of(q * PP + (p + kp) % PP, y), t)

    def x_peer(kx):
        return (f, ((x + kx) % X) * CORES + c)

    sibling = (f, x * CORES + 1 - c)
    sent = []

    def send(src, dst, s_sem, r_sem, device):
        d = pltpu.make_async_remote_copy(
            src_ref=src, dst_ref=dst, send_sem=s_sem, recv_sem=r_sem,
            device_id=device, device_id_type=MESH,
        )
        d.start()
        sent.append(d)

    def arrived(dst, s_sem, r_sem):
        pltpu.make_async_remote_copy(
            src_ref=dst, dst_ref=dst, send_sem=s_sem, recv_sem=r_sem,
            device_id=sibling, device_id_type=MESH,
        ).wait_recv()

    barrier = pltpu.get_barrier_semaphore()
    peers = [(fs_of((z + k) % Z, y), t) for k in range(1, Z)]
    peers += [(fs_of(z, (y + j) % Y), t) for j in range(1, Y)]
    peers += [x_peer(k) for k in range(1, X)] + [sibling]
    for peer in peers:
        pl.semaphore_signal(barrier, inc=1, device_id=peer, device_id_type=MESH)
    pl.semaphore_wait(barrier, len(peers))

    def z_send(layer, kind):
        for k in range(1, Z):
            dz = (z + k) % Z
            send(half_of(kind, layer, dz % PP), alls[kind].at[layer, f],
                 zs.at[layer, kind, k], zr.at[layer, kind, k], (fs_of(dz, y), t))

    def y_send(layer, kind, k):
        slot = fs_of((z - k + Z) % Z, y)
        src = half_of(kind, layer, p) if k == 0 else alls[kind].at[layer, slot]
        if k:
            arrived(alls[kind].at[layer, slot], zs.at[layer, kind, k], zr.at[layer, kind, k])
        for j in range(1, Y):
            send(src, alls[kind].at[layer, slot],
                 ys.at[layer, kind, k, j], yr.at[layer, kind, k, j],
                 (fs_of(z, (y + j) % Y), t))

    def y_wait(layer, kind):
        for k in range(Z):
            for j in range(1, Y):
                slot = fs_of((z - k + Z) % Z, (y - j + Y) % Y)
                arrived(alls[kind].at[layer, slot],
                        ys.at[layer, kind, k, j], yr.at[layer, kind, k, j])

    def forward(layer, kind):
        for k in range(1, Z):
            y_send(layer, kind, k)

    locals_ = []

    def keep_own(layer):
        for kind in range(2):
            d = pltpu.make_async_copy(half_of(kind, layer, p), alls[kind].at[layer, f],
                                      loc.at[layer, kind])
            d.start()
            locals_.append(d)

    half = rows // 2

    def tok_at(phase, h, kp, kx, core):
        g = (((p - kp + PP) % PP) * X + (x - kx + X) % X) * CORES + core
        return tok.at[phase, pl.ds(pl.multiple_of(g * rows + h * half, half), half)]

    def gather_x(phase, h, kp):
        for kx in range(1, X):
            send(tok_at(phase, h, kp, 0, c), tok_at(phase, h, kp, 0, c),
                 gxs.at[phase, h, kp, kx], gxr.at[phase, h, kp, kx], x_peer(kx))

    def gather_p(phase, h, kx):
        for kp in range(1, PP):
            send(tok_at(phase, h, 0, kx, c), tok_at(phase, h, 0, kx, c),
                 gps.at[phase, h, kp, kx], gpr.at[phase, h, kp, kx], p_peer(kp))

    def gather_c(phase, h, kp, kx):
        send(tok_at(phase, h, kp, kx, c), tok_at(phase, h, kp, kx, c),
             gcs.at[phase, h, kp, kx], gcr.at[phase, h, kp, kx], sibling)

    def got_x(phase, h, kp, kx):
        arrived(tok_at(phase, h, kp, kx, c), gxs.at[phase, h, kp, kx],
                gxr.at[phase, h, kp, kx])

    def got_p(phase, h, kp, kx):
        arrived(tok_at(phase, h, kp, kx, c), gps.at[phase, h, kp, kx],
                gpr.at[phase, h, kp, kx])

    def p_first(phase):
        return (0,) if phase else (0, 1)

    def x_first(phase):
        return (1,) if phase else ()

    def gather_start(phase):
        for h in p_first(phase):
            gather_p(phase, h, 0)
        for h in x_first(phase):
            gather_x(phase, h, 0)
            gather_p(phase, h, 0)
        for h in p_first(phase):
            gather_x(phase, h, 0)
        for h in range(2):
            gather_c(phase, h, 0, 0)

    def gather_relay(phase):
        for h in x_first(phase):
            for kx in range(1, X):
                got_x(phase, h, 0, kx)
                gather_p(phase, h, kx)
                gather_c(phase, h, 0, kx)
        for h in p_first(phase):
            for kp in range(1, PP):
                got_p(phase, h, kp, 0)
                gather_x(phase, h, kp)
                gather_c(phase, h, kp, 0)

    def gather_cross(phase):
        for h in p_first(phase):
            for kp in range(PP):
                for kx in range(1, X):
                    got_x(phase, h, kp, kx)
                    gather_c(phase, h, kp, kx)
        for h in x_first(phase):
            for kx in range(X):
                for kp in range(1, PP):
                    got_p(phase, h, kp, kx)
                    gather_c(phase, h, kp, kx)

    def gather_end(phase):
        for h in range(2):
            for kp in range(PP):
                for kx in range(X):
                    arrived(tok_at(phase, h, kp, kx, 1 - c),
                            gcs.at[phase, h, kp, kx], gcr.at[phase, h, kp, kx])

    both = CORES * rows
    chunk = both * math.gcd(PP * X, 2)

    def gate_up(layer):
        def step(i, carry):
            at = pl.ds(pl.multiple_of(i * chunk, chunk), chunk)
            weights = gu_all[layer].reshape(-1, 2 * HP)
            gu = jnp.dot(tok[layer, at, :], weights, preferred_element_type=jnp.float32)
            gate, value = gu[:, :HP], gu[:, HP:]
            hid[at, :] = (gate / (1.0 + jnp.exp(-gate)) * value).astype(jnp.bfloat16)
            return carry
        lax.fori_loop(0, PP * X * both // chunk, step, 0)

    order = sorted(((kp, kx) for kp in range(PP) for kx in range(X)),
                   key=lambda o: (o[1] == 0, o[0] == 0))
    top, low_half = pl.ds(0, half), pl.ds(half, half)

    def project_one(layer, kp, kx):
        o = kp * X + kx
        i = ((p + kp) % PP) * X + (x + kx) % X
        block = hid[pl.ds(pl.multiple_of(i * both, both), both), :][:, :H]
        down = jnp.concatenate([dn_all[layer, s] for s in range(Z * Y)], axis=1)
        res = jnp.dot(block, down, preferred_element_type=jnp.float32)
        low, high = res[:rows], res[rows:]
        part[o] = jnp.where(c == 0, low, high)
        psend[layer, o] = jnp.where(c == 0, high, low).astype(jnp.bfloat16)
        send(psend.at[layer, o], rcore.at[layer, o], rcs.at[layer, o], rcr.at[layer, o],
             sibling)

    def reduce_one(layer, kp, kx):
        o = kp * X + kx
        arrived(rcore.at[layer, o], rcs.at[layer, o], rcr.at[layer, o])
        total = part[o] + rcore[layer, o].astype(jnp.float32)
        part[o] = total
        if kp or kx:
            sums[layer, o] = total.astype(jnp.bfloat16)
        for h, at in enumerate((top, low_half)):
            first = kx if h in p_first(layer) else kp
            if first:
                send(sums.at[layer, o, at], rx.at[layer, o, at], rxs.at[layer, h, o],
                     rxr.at[layer, h, o],
                     x_peer(kx) if h in p_first(layer) else p_peer(kp))

    def project(layer):
        for n, (kp, kx) in enumerate(order):
            project_one(layer, kp, kx)
            if n:
                reduce_one(layer, *order[n - 1])
        reduce_one(layer, *order[-1])

    def first_sum(layer, h, at, keep, others):
        total = part[keep, at, :]
        for o in others:
            arrived(rx.at[layer, o, at], rxs.at[layer, h, o], rxr.at[layer, h, o])
            total = total + rx[layer, o, at, :].astype(jnp.float32)
        return total

    def second_send(layer, h, at, n, total, device):
        up_sum[layer, n, at, :] = total.astype(jnp.bfloat16)
        send(up_sum.at[layer, n, at], rp.at[layer, n, at], rps.at[layer, h, n],
             rpr.at[layer, h, n], device)

    def reduce_x(layer):
        for h, at in enumerate((top, low_half)):
            straight = h in p_first(layer)
            for n in reversed(range(PP if straight else X)):
                if straight:
                    keep, others = n * X, [n * X + kx for kx in range(1, X)]
                else:
                    keep, others = n, [kp * X + n for kp in range(1, PP)]
                total = first_sum(layer, h, at, keep, others)
                if n:
                    second_send(layer, h, at, n, total, p_peer(n) if straight else x_peer(n))
                else:
                    part[0, at, :] = total

    def reduce_p(layer):
        def last(h, at):
            total = part[0, at, :]
            for n in range(1, PP if h in p_first(layer) else X):
                arrived(rp.at[layer, n, at], rps.at[layer, h, n], rpr.at[layer, h, n])
                total = total + rp[layer, n, at, :].astype(jnp.float32)
            return total.astype(jnp.bfloat16)
        return jnp.concatenate([last(0, top), last(1, low_half)], axis=0)

    own_rows = pl.ds(pl.multiple_of(((p * X + x) * CORES + c) * rows, rows), rows)

    loads[0].wait()
    tok[0, own_rows, :] = rms_rows(stream_ref[...], gains_ref[0:1, :])
    gather_start(0)
    loads[1].wait()
    loads[2].wait()
    pack(0)
    z_send(0, 0)
    y_send(0, 0, 0)
    z_send(0, 1)
    y_send(0, 1, 0)
    keep_own(0)
    loads[3].wait()
    loads[4].wait()
    pack(1)
    z_send(1, 0)
    z_send(1, 1)
    keep_own(1)
    gather_relay(0)
    gather_cross(0)
    forward(0, 0)
    gather_end(0)
    forward(0, 1)
    y_send(1, 0, 0)
    y_send(1, 1, 0)
    loads[5].wait()
    for d in locals_:
        d.wait()
    y_wait(0, 0)
    gate_up(0)
    y_wait(0, 1)
    project(0)
    forward(1, 0)
    reduce_x(0)
    forward(1, 1)
    branch = reduce_p(0)
    after_first = add_branch(
        stream_ref[...], rms_rows(branch, gains_ref[1:2, :]), half_weight
    )
    joined = add_branch(after_first, rms_rows(mixer_ref[...], mixer_gain_ref[...]), 1.0)
    mixed[...] = joined
    tok[1, own_rows, :] = rms_rows(joined, gains_ref[2:3, :])
    gather_start(1)
    gather_relay(1)
    gather_cross(1)
    gather_end(1)
    y_wait(1, 0)
    gate_up(1)
    y_wait(1, 1)
    project(1)
    reduce_x(1)
    branch_two = reduce_p(1)
    out_ref[...] = add_branch(
        mixed[...], rms_rows(branch_two, gains_ref[3:4, :]), half_weight
    )
    for d in sent:
        d.wait_send()


def on_device(sizes, stream, mixer_out, ffn_gains, mixer_gain,
              gate_first, up_first, down_first, gate_second, up_second, down_second):
    n_fs, n_tp = sizes
    X = n_tp // CORES
    Y = math.gcd(n_fs, X)
    Z = n_fs // Y
    PP = math.gcd(Z, PAIR)
    depth, local_h = gate_first.shape
    H = local_h // PP
    HP = -(-H // 128) * 128
    rows, width = stream.shape

    group = PP * X
    most = max(PP, X)
    bf, f32 = jnp.bfloat16, jnp.float32
    dma = pltpu.SemaphoreType.DMA
    vm = pltpu.VMEM
    F = n_fs
    any_ = pl.ANY
    scratch = [
        vm((rows, width), bf), vm((rows, width), bf), vm((2, 2, depth, local_h), bf),
        vm((2, PP, depth, 2 * HP), bf),
        vm((2, F, depth, 2 * HP), bf), vm((2, F, H, depth), bf),
        vm((2, group * CORES * rows, width), bf), vm((group * CORES * rows, HP), bf),
        vm((group, rows, width), f32), vm((2, group, rows, width), bf),
        vm((2, group, rows, width), bf), vm((2, group, rows, width), bf),
        vm((2, group, rows, width), bf), vm((2, most, rows, width), bf),
        vm((2, most, rows, width), bf), vm((rows, width), bf),
        dma((2, 2, Z)), dma((2, 2, Z)), dma((2, 2, Z, Y)), dma((2, 2, Z, Y)),
        dma((2, 2, PP, X)), dma((2, 2, PP, X)), dma((2, 2, PP, X)), dma((2, 2, PP, X)),
        dma((2, 2, PP, X)), dma((2, 2, PP, X)), dma((2, group)), dma((2, group)),
        dma((2, 2, group)), dma((2, 2, group)), dma((2, 2, most)), dma((2, 2, most)),
        dma((2, 2)), dma((6,)),
    ]
    return pl.pallas_call(
        functools.partial(layer_kernel, (Z, Y, X, PP, H, HP)),
        out_shape=jax.ShapeDtypeStruct((rows, width), bf),
        in_specs=[pl.BlockSpec(memory_space=m) for m in (any_, any_, vm, vm) + (any_,) * 6],
        out_specs=pl.BlockSpec(memory_space=vm),
        scratch_shapes=scratch,
        compiler_params=pltpu.CompilerParams(collective_id=0, has_side_effects=True),
        name="macaron",
    )(stream, mixer_out, ffn_gains, mixer_gain.reshape(1, -1),
      gate_first, up_first, down_first, gate_second, up_second, down_second)


def solution(mesh):
    in_specs = (
        P(("fs", "tp"), None), P(("fs", "tp"), None), P(), P(),
        P("fs", "tp"), P("fs", "tp"), P("tp", "fs"),
        P("fs", "tp"), P("fs", "tp"), P("tp", "fs"),
    )
    sizes = (mesh.shape["fs"], mesh.shape["tp"])
    return jax.shard_map(
        functools.partial(on_device, sizes), mesh=mesh, in_specs=in_specs,
        out_specs=P(("fs", "tp"), None), check_vma=False,
    )
```
